768 devices in a mesh: sp: 16 (over y, core), dp: 48 (over z, x).
Axes of the slice: x: 4, y: 8, z: 12, core: 2. Of those that a mesh axis runs over, the one named last changes fastest.
Arguments:
- queries: bfloat16 [48, 4096, 1024], P('dp', 'sp'), may hold values from -250 to 250
- keys: bfloat16 [48, 4096, 1024], P('dp', 'sp'), may hold values from -6 to 6
- values: bfloat16 [48, 4096, 1024], P('dp', 'sp'), may hold values from -6 to 6
- cum_gate: float32 [48, 16, 4096], P('dp', 'sp'), may hold values from -4096 to 0, as said below
- out_weight: bfloat16 [1024, 2112], P(None, 'dp'), may hold values from -1.5 to 1.5
Outputs:
- mixed: bfloat16 [48, 4096, 2112], P('dp', 'sp')
The draws below stay inside these ranges and needn't reach their ends.
Inputs may be any that keep to these rules, and one draw needn't show every extreme that they name: `cum_gate`: within each head the entries do not rise along positions.
All inputs are finite; a program needn't handle non-finite values.
Results may differ from the reference program's by a relative error of at most 0.0053.
Values may be sent and summed in bfloat16 or wider, within the bound.
No kernel may reach another device: no remote copies, remote signals or barrier semaphores. Data moves between devices by JAX's collectives and lax.ppermute only.
A program may use at most 64 MiB of HBM per device.

```python
import jax
import jax.numpy as jnp
from jax import lax

D = 2112
HEAD_COUNT = 16
HEAD_DIM = 64
TOK_DEV = 256
WIDTH = 1024
SEQUENCE_LENGTH = 4096
SEQUENCE_COUNT = 48


def drawn_pair(key):
    key_query, key_key = jax.random.split(jax.random.fold_in(key, 11), 2)
    query_draw = 1.5 * jnp.clip(jax.random.normal(key_query, (SEQUENCE_COUNT, SEQUENCE_LENGTH, WIDTH), jnp.float32), -6.0, 6.0)
    key_draw = jnp.clip(jax.random.normal(key_key, (SEQUENCE_COUNT, SEQUENCE_LENGTH, WIDTH), jnp.float32), -6.0, 6.0)
    return (query_draw, key_draw)


def draw_queries(key, part):
    return drawn_pair(key)[0].astype(jnp.bfloat16)


def draw_keys(key, part):
    return drawn_pair(key)[1].astype(jnp.bfloat16)


def draw_values(key, part):
    base = jax.random.normal(jax.random.fold_in(key, 31), (SEQUENCE_COUNT, SEQUENCE_LENGTH, WIDTH), jnp.float32)
    return jnp.clip(base, -6.0, 6.0).astype(jnp.bfloat16)


def draw_cum_gate(key, part):
    key_heads, key_slow, key_fast, key_block, key_rough, key_place, key_loss = jax.random.split(jax.random.fold_in(key, 23), 7)
    head_order = jax.random.permutation(key_heads, HEAD_COUNT)
    sluggish_head = head_order < HEAD_COUNT // 2
    sluggish_head = sluggish_head[None, :, None]
    slow_rate = jax.random.uniform(key_slow, (SEQUENCE_COUNT, HEAD_COUNT, 1), jnp.float32, 0.3, 1.0) / SEQUENCE_LENGTH
    fast_rate = jax.random.uniform(key_fast, (SEQUENCE_COUNT, HEAD_COUNT, 1), jnp.float32, 1.0 / 100.0, 1.0 / 30.0)
    baseline_decay = jnp.where(sluggish_head, slow_rate, fast_rate)
    shard_count = SEQUENCE_LENGTH // TOK_DEV
    block_multiplier = jnp.exp(jax.random.uniform(key_block, (SEQUENCE_COUNT, HEAD_COUNT, shard_count, 1), jnp.float32, jnp.log(0.5), jnp.log(2.0)))
    block_multiplier = jnp.broadcast_to(block_multiplier, (SEQUENCE_COUNT, HEAD_COUNT, shard_count, TOK_DEV)).reshape(SEQUENCE_COUNT, HEAD_COUNT, SEQUENCE_LENGTH)
    jitter_level = jax.random.uniform(key_rough, (SEQUENCE_COUNT, HEAD_COUNT, SEQUENCE_LENGTH), jnp.float32, 0.3, 1.7)
    spike_locations = jax.random.randint(key_place, (SEQUENCE_COUNT, HEAD_COUNT, 3), 0, SEQUENCE_LENGTH)
    decay_amounts = jax.random.uniform(key_loss, (SEQUENCE_COUNT, HEAD_COUNT, 3), jnp.float32, 0.22, 0.5)
    token_positions = jnp.arange(SEQUENCE_LENGTH, dtype=jnp.int32)
    spike_events = jnp.zeros((SEQUENCE_COUNT, HEAD_COUNT, SEQUENCE_LENGTH), jnp.float32)
    for spike_event in range(3):
        spike_events = spike_events + jnp.where(token_positions[None, None, :] == spike_locations[:, :, spike_event:spike_event + 1], decay_amounts[:, :, spike_event:spike_event + 1], 0.0)
    gate_logarithm = -baseline_decay * block_multiplier * jitter_level - jnp.where(sluggish_head, spike_events, 0.0)
    return jnp.cumsum(gate_logarithm, axis=-1)


def levels(stream_key, shape, cuts, low, top_value):
    loudness = 1.0
    for dim, blocks in cuts:
        steps = jax.random.uniform(jax.random.fold_in(jax.random.fold_in(stream_key, 6), dim), (blocks,), jnp.float32, low / len(cuts), top_value / len(cuts))
        loudness = loudness * jnp.repeat(jnp.exp(steps), shape[dim] // blocks).reshape((-1,) + (1,) * (len(shape) - 1 - dim))
    return loudness


def normal_values(key, dims, scale, most, shards=(), kind=jnp.bfloat16):
    array = scale * jax.random.normal(key, dims, jnp.float32)
    if shards:
        array = array * levels(key, dims, shards, -0.22, 0.18)
    return jnp.clip(array, -most, most).astype(kind)


def setup_inputs(seed: int = 0) -> dict:
    key_list = jax.random.split(jax.random.key(seed), 6)
    queries = draw_queries(jax.random.fold_in(key_list[5], 71), 0)
    keys = draw_keys(jax.random.fold_in(key_list[5], 71), 0)
    values = draw_values(jax.random.fold_in(key_list[5], 71), 0)
    cum_gate = draw_cum_gate(jax.random.fold_in(key_list[5], 71), 0)
    out_weight = normal_values(key_list[4], (WIDTH, D), (WIDTH // 64) ** -0.5, 1.5, ((1, 48),))
    return {"queries": queries, "keys": keys, "values": values, "cum_gate": cum_gate, "out_weight": out_weight}


def reference(queries, keys, values, cum_gate, out_weight):
    sequences, length, width = queries.shape
    block_rows = min(512, length)
    block_count = length // block_rows
    score_scale = HEAD_DIM ** -0.5
    token_positions = jnp.arange(length, dtype=jnp.int32)

    def one_sequence(arrays):
        query_seq, key_seq, value_seq, gate_seq = arrays
        query_f = query_seq.astype(jnp.float32).reshape(length, HEAD_COUNT, HEAD_DIM)
        key_f = key_seq.astype(jnp.float32).reshape(length, HEAD_COUNT, HEAD_DIM)
        value_f = value_seq.astype(jnp.float32).reshape(length, HEAD_COUNT, HEAD_DIM)

        def one_block(block_index):
            first_row = (block_index * block_rows).astype(jnp.int32)
            query_part = lax.dynamic_slice_in_dim(query_f, first_row, block_rows, 0)
            gate_part = lax.dynamic_slice_in_dim(gate_seq, first_row, block_rows, 1)
            logits = jnp.einsum('qhe,khe->hqk', query_part, key_f) * score_scale
            logits = logits + gate_part[:, :, None] - gate_seq[:, None, :]
            query_rows = first_row + jnp.arange(block_rows, dtype=jnp.int32)
            allowed = token_positions[None, None, :] <= query_rows[None, :, None]
            logits = jnp.where(allowed, logits, -jnp.inf)
            scores = jnp.exp(logits - jnp.max(logits, axis=-1, keepdims=True))
            denominator = jnp.sum(scores, axis=-1)
            scores_low = lax.optimization_barrier(scores.astype(jnp.bfloat16)).astype(jnp.float32)
            weighted = jnp.einsum('hqk,khe->hqe', scores_low, value_f) / denominator[..., None]
            return weighted.transpose(1, 0, 2).reshape(block_rows, width).astype(jnp.bfloat16)

        blocks = lax.map(one_block, jnp.arange(block_count, dtype=jnp.int32))
        return blocks.reshape(length, width)

    attended = lax.map(one_sequence, (queries, keys, values, cum_gate))
    mixed = jnp.dot(attended.reshape(sequences * length, width), out_weight,
                    preferred_element_type=jnp.float32)
    return mixed.astype(jnp.bfloat16).reshape(sequences, length, out_weight.shape[1])
```

```python
import math

import jax
import jax.numpy as jnp
from jax import lax
from jax.experimental import pallas as pl
from jax.experimental.pallas import tpu as pltpu
from jax.sharding import Mesh
from jax.sharding import PartitionSpec as P

SP = ("sp_0", "sp_1")
LOG2E = math.log2(math.e)
VMEM = pl.BlockSpec(memory_space=pltpu.VMEM)
SMEM = pl.BlockSpec(memory_space=pltpu.SMEM)


def swap_halves(a):
    return jnp.concatenate([a[:, 64:], a[:, :64]], axis=1)


def low_lanes(shape):
    return lax.broadcasted_iota(jnp.int32, shape, 1) < 64


def interleave(first, second):
    lanes = low_lanes(first.shape)
    return (
        jnp.where(lanes, first, swap_halves(second)),
        jnp.where(lanes, swap_halves(first), second),
    )


def pack_kernel(queries, keys, values, out):
    for t, ref in enumerate((queries, keys, values)):
        for j in range(out.shape[0] // 2):
            columns = slice(128 * j, 128 * j + 128)
            out[2 * j, t], out[2 * j + 1, t] = interleave(ref[0:128, columns], ref[128:256, columns])


def pack(queries, keys, values):
    rows, width = queries.shape
    heads, steps = width // 64, 4
    return pl.pallas_call(
        pack_kernel,
        grid=(steps,),
        out_shape=jax.ShapeDtypeStruct((heads, 3, rows // 2, 128), jnp.bfloat16),
        in_specs=[pl.BlockSpec((rows, width // steps), lambda i: (0, i))] * 3,
        out_specs=pl.BlockSpec((heads // steps, 3, rows // 2, 128), lambda i: (i, 0, 0, 0)),
        cost_estimate=pl.CostEstimate(flops=1_000_000, bytes_accessed=3_000_000, transcendentals=0),
        compiler_params=pltpu.CompilerParams(vmem_limit_bytes=8 * 2**20),
        name="pack",
    )(queries, keys, values)


def gate_kernel(gate, out):
    row = lax.broadcasted_iota(jnp.int32, (8, 128), 0)
    for n in range(gate.shape[0]):
        g = jnp.broadcast_to(gate[n : n + 1, :] * -LOG2E, (8, 128))
        high = g.astype(jnp.bfloat16).astype(jnp.float32)
        rest = g - high
        middle = rest.astype(jnp.bfloat16).astype(jnp.float32)
        low = rest - middle
        rows = jnp.where(row == 0, high, jnp.where(row == 1, middle, jnp.where(row == 2, low, 0.0)))
        tile = jnp.concatenate(
            [jnp.zeros((64, 128), jnp.float32), rows, jnp.zeros((56, 128), jnp.float32)], axis=0
        )
        out[128 * n : 128 * n + 128, :] = tile.T.astype(jnp.bfloat16)


def gate_columns(gate):
    return pl.pallas_call(
        gate_kernel,
        out_shape=jax.ShapeDtypeStruct((gate.size, 128), jnp.bfloat16),
        in_specs=[VMEM],
        out_specs=VMEM,
        cost_estimate=pl.CostEstimate(flops=10_000_000, bytes_accessed=1_000_000, transcendentals=0),
        compiler_params=pltpu.CompilerParams(vmem_limit_bytes=6 * 2**20),
        name="gate_columns",
    )(gate)


def attend_kernel(parts, gate, out, keys, values, logits):
    count = parts.shape[0]
    lanes = low_lanes((128, 128))
    values[64:80, :] = jnp.ones((16, values.shape[1]), jnp.bfloat16)
    for b in range(count):
        base = 256 * b
        k = parts[b, 1]
        swapped = swap_halves(k)
        keys[base : base + 128, 0:128] = jnp.where(lanes, k, swapped)
        keys[base + 128 : base + 256, 0:128] = jnp.where(lanes, swapped, k)
        keys[base : base + 128, 128:256] = jnp.where(lanes, k, gate[base : base + 128, :])
        keys[base + 128 : base + 256, 128:256] = jnp.where(
            lanes, swapped, gate[base + 128 : base + 256, :]
        )
        v = parts[b, 2].T
        values[0:64, base : base + 128] = v[:64]
        values[0:64, base + 128 : base + 256] = v[64:]
    causal = lax.broadcasted_iota(jnp.int32, (256, 256), 0) <= lax.broadcasted_iota(
        jnp.int32, (256, 256), 1
    )

    def first(i):
        q = parts[i, 0].astype(jnp.float32).T
        q = jnp.concatenate([q[:64], q[64:]], axis=1) * (LOG2E / 8.0)
        high = q.astype(jnp.bfloat16)
        rest = q - high.astype(jnp.float32)
        middle = rest.astype(jnp.bfloat16)
        low = (rest - middle.astype(jnp.float32)).astype(jnp.bfloat16)
        queries = jnp.concatenate([high, middle, low, jnp.ones((64, 256), jnp.bfloat16)], axis=0)
        peak = None
        for j in range(i + 1):
            s = jnp.dot(
                keys[256 * j : 256 * j + 256, :], queries, preferred_element_type=jnp.float32
            )
            if j == i:
                s = jnp.where(causal, s, -jnp.inf)
            logits[i % 2, 256 * j : 256 * j + 256, :] = s
            top = jnp.max(s.reshape(32, 8, 256), axis=0)
            peak = top if peak is None else jnp.maximum(peak, top)
        return jnp.max(peak, axis=0, keepdims=True)

    def second(i, peak):
        total = None
        for j in range(i + 1):
            p = jnp.exp2(logits[i % 2, 256 * j : 256 * j + 256, :] - peak).astype(jnp.bfloat16)
            o = jnp.dot(
                values[:, 256 * j : 256 * j + 256], p, preferred_element_type=jnp.float32
            )
            total = o if total is None else total + o
        out[i] = (total[:64] / total[64:65]).astype(jnp.bfloat16)

    peak = first(0)
    for i in range(count):
        following = first(i + 1) if i + 1 < count else None
        second(i, peak)
        peak = following


def attend(parts, gate):
    count = parts.shape[0]
    length = 256 * count
    return pl.pallas_call(
        attend_kernel,
        out_shape=jax.ShapeDtypeStruct((count, 64, 256), jnp.bfloat16),
        in_specs=[VMEM] * 2,
        out_specs=VMEM,
        scratch_shapes=[
            pltpu.VMEM((length, 256), jnp.bfloat16),
            pltpu.VMEM((80, length), jnp.bfloat16),
            pltpu.VMEM((2, length, 256), jnp.float32),
        ],
        compiler_params=pltpu.CompilerParams(vmem_limit_bytes=32 * 2**20),
        cost_estimate=pl.CostEstimate(
            flops=10_000_000_000, bytes_accessed=4_000_000, transcendentals=9_000_000
        ),
        name="attend",
    )(parts, gate)


def assemble_kernel(me, blocks, out):
    x = me[0]
    hops, groups, columns, _ = blocks.shape
    for k in range(hops):
        hop = lax.rem(x - k + hops, hops)
        for z in range(groups):
            row = columns * (hops * z + k)
            out[row : row + columns, :] = blocks[hop, z]


def assemble(me, blocks):
    hops, groups, columns, depth = blocks.shape
    return pl.pallas_call(
        assemble_kernel,
        out_shape=jax.ShapeDtypeStruct((hops * groups * columns, depth), jnp.bfloat16),
        in_specs=[SMEM, VMEM],
        out_specs=VMEM,
        cost_estimate=pl.CostEstimate(flops=1_000_000, bytes_accessed=4_300_000, transcendentals=0),
        compiler_params=pltpu.CompilerParams(vmem_limit_bytes=16 * 2**20),
        name="assemble",
    )(me, blocks)


def project_kernel(core, attended, mine, other, out):
    heads, depth, rows = attended.shape
    c, half = core[0], heads // 2

    def columns(first):
        return attended[pl.ds(first, half)].reshape(half * depth, rows)

    total = jnp.dot(mine[...], columns(c * half), preferred_element_type=jnp.float32)
    total += jnp.dot(other[...], columns((1 - c) * half), preferred_element_type=jnp.float32)
    out[...] = total.astype(jnp.bfloat16)


def project(core, attended, mine, other):
    columns = mine.shape[0]
    return pl.pallas_call(
        project_kernel,
        out_shape=jax.ShapeDtypeStruct((columns, attended.shape[2]), jnp.bfloat16),
        in_specs=[SMEM] + [VMEM] * 3,
        out_specs=VMEM,
        compiler_params=pltpu.CompilerParams(vmem_limit_bytes=16 * 2**20),
        cost_estimate=pl.CostEstimate(
            flops=1_100_000_000, bytes_accessed=6_000_000, transcendentals=0
        ),
        name="project",
    )(core, attended, mine, other)


def body(queries, keys, values, cum_gate, out_weight):
    core, x = lax.axis_index("sp_1"), lax.axis_index("x")
    packed = pack(queries[0], keys[0], values[0])
    parts = lax.all_to_all(packed, SP, 0, 0, tiled=True)
    gate = gate_columns(cum_gate[0, 0].reshape(-1, 128))

    depth = out_weight.shape[0] // 2
    own = lax.dynamic_slice_in_dim(out_weight.T, core * depth, depth, axis=1)
    along_z = lax.all_gather(own[None], "z", axis=0, tiled=True)
    n = lax.axis_size("x")
    blocks = [along_z] + [
        lax.ppermute(along_z, "x", [(i, (i + hop) % n) for i in range(n)]) for hop in range(1, n)
    ]
    mine = assemble(x.reshape(1), jnp.stack(blocks))
    other = lax.ppermute(mine, "sp_1", [(0, 1), (1, 0)])

    local = attend(parts, gate)
    back = lax.all_to_all(local, SP, 0, 0, tiled=True)
    return project(core.reshape(1), back, mine, other).T[None]


def solution(mesh):
    split = Mesh(mesh.devices.reshape(8, 2, 12, 4), ("sp_0", "sp_1", "z", "x"))
    dp = ("z", "x")
    return jax.shard_map(
        body,
        mesh=split,
        in_specs=(P(dp, SP, None), P(dp, SP, None), P(dp, SP, None), P(dp, SP, None), P(None, dp)),
        out_specs=P(dp, SP, None),
        check_vma=False,
    )
```

```python
import math

import jax
import jax.numpy as jnp
from jax import lax
from jax.experimental import pallas as pl
from jax.experimental.pallas import tpu as pltpu
from jax.sharding import Mesh
from jax.sharding import PartitionSpec as P


SP = ("sp_0", "sp_1")
LOG2E = math.log2(math.e)
VMEM = pl.BlockSpec(memory_space=pltpu.VMEM)
SMEM = pl.BlockSpec(memory_space=pltpu.SMEM)
HBM = pl.BlockSpec(memory_space=pltpu.HBM)


def swap_halves(a):
    return jnp.concatenate([a[:, 64:], a[:, :64]], axis=1)


def low_lanes(shape):
    return lax.broadcasted_iota(jnp.int32, shape, 1) < 64


def interleave(first, second):
    lanes = low_lanes(first.shape)
    return (
        jnp.where(lanes, first, swap_halves(second)),
        jnp.where(lanes, swap_halves(first), second),
    )


def pack_kernel(queries, keys, values, out, taken, packed, arrived, left):
    heads = out.shape[0]
    groups = arrived.shape[0]
    width, each = taken.shape[2] // groups, heads // groups

    def arrival(g, t):
        columns = slice(width * g, width * g + width)
        source = (queries, keys, values)[t]
        return pltpu.make_async_copy(
            source.at[:, columns], taken.at[t, :, columns], arrived.at[g, t]
        )

    def departure(g):
        block = slice(each * g, each * g + each)
        return pltpu.make_async_copy(packed.at[block], out.at[block], left.at[g])

    for g in range(groups):
        for t in range(3):
            arrival(g, t).start()
    for g in range(groups):
        for t in range(3):
            arrival(g, t).wait()
            for j in range(each * g // 2, (each * g + each) // 2):
                columns = slice(128 * j, 128 * j + 128)
                packed[2 * j, t], packed[2 * j + 1, t] = interleave(
                    taken[t, 0:128, columns], taken[t, 128:256, columns]
                )
        departure(g).start()
    for g in range(groups):
        departure(g).wait()


def pack(queries, keys, values):
    rows, width = queries.shape
    heads, groups = width // 64, 4
    return pl.pallas_call(
        pack_kernel,
        out_shape=jax.ShapeDtypeStruct((heads, 3, rows // 2, 128), jnp.bfloat16),
        in_specs=[HBM] * 3,
        out_specs=HBM,
        scratch_shapes=[
            pltpu.VMEM((3, rows, width), jnp.bfloat16),
            pltpu.VMEM((heads, 3, rows // 2, 128), jnp.bfloat16),
            pltpu.SemaphoreType.DMA((groups, 3)),
            pltpu.SemaphoreType.DMA((groups,)),
        ],
        compiler_params=pltpu.CompilerParams(vmem_limit_bytes=60 * 2**20),
        cost_estimate=pl.CostEstimate(flops=1_000_000, bytes_accessed=3_000_000, transcendentals=0),
        name="pack",
    )(queries, keys, values)


def gate_kernel(gate, out):
    row = lax.broadcasted_iota(jnp.int32, (8, 128), 0)
    for n in range(gate.shape[0]):
        g = jnp.broadcast_to(gate[n : n + 1, :] * -LOG2E, (8, 128))
        high = g.astype(jnp.bfloat16).astype(jnp.float32)
        rest = g - high
        middle = rest.astype(jnp.bfloat16).astype(jnp.float32)
        low = rest - middle
        rows = jnp.where(row == 0, high, jnp.where(row == 1, middle, jnp.where(row == 2, low, 0.0)))
        tile = jnp.concatenate(
            [jnp.zeros((64, 128), jnp.float32), rows, jnp.zeros((56, 128), jnp.float32)], axis=0
        )
        out[128 * n : 128 * n + 128, :] = tile.T.astype(jnp.bfloat16)


def gate_columns(gate):
    return pl.pallas_call(
        gate_kernel,
        out_shape=jax.ShapeDtypeStruct((gate.size, 128), jnp.bfloat16),
        in_specs=[VMEM],
        out_specs=VMEM,
        cost_estimate=pl.CostEstimate(flops=10_000_000, bytes_accessed=1_000_000, transcendentals=0),
        compiler_params=pltpu.CompilerParams(vmem_limit_bytes=6 * 2**20),
        name="gate_columns",
    )(gate)


def attend_kernel(source, columns, out, parts, gate, keys, values, logits, finished, arrived, left):
    count = parts.shape[0]

    def arrival(b):
        rows = slice(256 * b, 256 * b + 256)
        return (
            pltpu.make_async_copy(source.at[b], parts.at[b], arrived.at[b, 0]),
            pltpu.make_async_copy(columns.at[rows], gate.at[rows], arrived.at[b, 1]),
        )

    def departure(b):
        return pltpu.make_async_copy(finished.at[b], out.at[b], left.at[b])

    for b in range(count):
        for copy in arrival(b):
            copy.start()
    lanes = low_lanes((128, 128))
    values[64:80, :] = jnp.ones((16, values.shape[1]), jnp.bfloat16)
    for b in range(count):
        base = 256 * b
        for copy in arrival(b):
            copy.wait()
        k = parts[b, 1]
        swapped = swap_halves(k)
        keys[base : base + 128, 0:128] = jnp.where(lanes, k, swapped)
        keys[base + 128 : base + 256, 0:128] = jnp.where(lanes, swapped, k)
        keys[base : base + 128, 128:256] = jnp.where(lanes, k, gate[base : base + 128, :])
        keys[base + 128 : base + 256, 128:256] = jnp.where(
            lanes, swapped, gate[base + 128 : base + 256, :]
        )
        v = parts[b, 2].T
        values[0:64, base : base + 128] = v[:64]
        values[0:64, base + 128 : base + 256] = v[64:]
    causal = lax.broadcasted_iota(jnp.int32, (256, 256), 0) <= lax.broadcasted_iota(
        jnp.int32, (256, 256), 1
    )

    def first(i):
        q = parts[i, 0].astype(jnp.float32).T
        q = jnp.concatenate([q[:64], q[64:]], axis=1) * (LOG2E / 8.0)
        high = q.astype(jnp.bfloat16)
        rest = q - high.astype(jnp.float32)
        middle = rest.astype(jnp.bfloat16)
        low = (rest - middle.astype(jnp.float32)).astype(jnp.bfloat16)
        queries = jnp.concatenate([high, middle, low, jnp.ones((64, 256), jnp.bfloat16)], axis=0)
        peak = None
        for j in range(i + 1):
            s = jnp.dot(
                keys[256 * j : 256 * j + 256, :], queries, preferred_element_type=jnp.float32
            )
            if j == i:
                s = jnp.where(causal, s, -jnp.inf)
            logits[i % 2, 256 * j : 256 * j + 256, :] = s
            top = jnp.max(s.reshape(32, 8, 256), axis=0)
            peak = top if peak is None else jnp.maximum(peak, top)
        return jnp.max(peak, axis=0, keepdims=True)

    def second(i, peak):
        total = None
        for j in range(i + 1):
            p = jnp.exp2(logits[i % 2, 256 * j : 256 * j + 256, :] - peak).astype(jnp.bfloat16)
            o = jnp.dot(
                values[:, 256 * j : 256 * j + 256], p, preferred_element_type=jnp.float32
            )
            total = o if total is None else total + o
        finished[i] = (total[:64] / total[64:65]).astype(jnp.bfloat16)
        departure(i).start()

    peak = first(0)
    for i in range(count):
        following = first(i + 1) if i + 1 < count else None
        second(i, peak)
        peak = following
    for i in range(count):
        departure(i).wait()


def attend(parts, gate):
    count = parts.shape[0]
    length = 256 * count
    return pl.pallas_call(
        attend_kernel,
        out_shape=jax.ShapeDtypeStruct((count, 64, 256), jnp.bfloat16),
        in_specs=[HBM, HBM],
        out_specs=HBM,
        scratch_shapes=[
            pltpu.VMEM(parts.shape, jnp.bfloat16),
            pltpu.VMEM(gate.shape, jnp.bfloat16),
            pltpu.VMEM((length, 256), jnp.bfloat16),
            pltpu.VMEM((80, length), jnp.bfloat16),
            pltpu.VMEM((2, length, 256), jnp.float32),
            pltpu.VMEM((count, 64, 256), jnp.bfloat16),
            pltpu.SemaphoreType.DMA((count, 2)),
            pltpu.SemaphoreType.DMA((count,)),
        ],
        compiler_params=pltpu.CompilerParams(vmem_limit_bytes=60 * 2**20),
        cost_estimate=pl.CostEstimate(
            flops=10_000_000_000, bytes_accessed=4_000_000, transcendentals=9_000_000
        ),
        name="attend",
    )(parts, gate)


def assemble_kernel(me, after, *refs):
    del after
    *blocks, out = refs
    hops = len(blocks)
    groups, columns, _ = blocks[0].shape
    for k in range(hops):
        for hop in range(hops):

            @pl.when(lax.rem(me[0] - k + hops, hops) == hop)
            def _():
                @pl.loop(0, groups)
                def _(z):
                    first = pl.multiple_of(hops * columns * z, 8)
                    group = out.at[pl.ds(first, hops * columns)]
                    group[columns * k : columns * k + columns, :] = blocks[hop][z]


def assemble(me, after, blocks):
    groups, columns, depth = blocks[0].shape
    return pl.pallas_call(
        assemble_kernel,
        out_shape=jax.ShapeDtypeStruct((len(blocks) * groups * columns, depth), jnp.bfloat16),
        in_specs=[SMEM, pl.BlockSpec(memory_space=pl.ANY)] + [VMEM] * len(blocks),
        out_specs=VMEM,
        compiler_params=pltpu.CompilerParams(vmem_limit_bytes=60 * 2**20),
        cost_estimate=pl.CostEstimate(flops=1_000_000, bytes_accessed=4_300_000, transcendentals=0),
        name="assemble",
    )(me, after, *blocks)


def project_kernel(core, attended, mine, other, out):
    heads, depth, rows = attended.shape
    c, half = core[0], heads // 2

    def columns(first):
        return attended[pl.ds(first, half)].reshape(half * depth, rows)

    total = jnp.dot(mine[...], columns(c * half), preferred_element_type=jnp.float32)
    total += jnp.dot(other[...], columns((1 - c) * half), preferred_element_type=jnp.float32)
    out[...] = total.astype(jnp.bfloat16)


def project(core, attended, mine, other):
    columns, step = mine.shape[0], 352
    return pl.pallas_call(
        project_kernel,
        out_shape=jax.ShapeDtypeStruct((columns, attended.shape[2]), jnp.bfloat16),
        grid=(columns // step,),
        in_specs=[
            SMEM,
            pl.BlockSpec(attended.shape, lambda i: (0, 0, 0)),
            pl.BlockSpec((step, mine.shape[1]), lambda i: (i, 0)),
            pl.BlockSpec((step, other.shape[1]), lambda i: (i, 0)),
        ],
        out_specs=pl.BlockSpec((step, attended.shape[2]), lambda i: (i, 0)),
        compiler_params=pltpu.CompilerParams(vmem_limit_bytes=16 * 2**20),
        cost_estimate=pl.CostEstimate(
            flops=1_100_000_000, bytes_accessed=6_000_000, transcendentals=0
        ),
        name="project",
    )(core, attended, mine, other)


def body(queries, keys, values, cum_gate, out_weight):
    core, x = lax.axis_index("sp_1"), lax.axis_index("x")
    packed = pack(queries[0], keys[0], values[0])
    parts = lax.all_to_all(packed, SP, 0, 0, tiled=True)
    gate = gate_columns(cum_gate[0, 0].reshape(-1, 128))

    depth = out_weight.shape[0] // 2
    own = lax.dynamic_slice_in_dim(out_weight.T, core * depth, depth, axis=1)
    along_z = lax.all_gather(own[None], "z", axis=0, tiled=True)
    n = lax.axis_size("x")
    blocks = [along_z] + [
        lax.ppermute(along_z, "x", [(i, (i + hop) % n) for i in range(n)])
        for hop in range(1, n)
    ]
    local = attend(parts, gate)
    mine = assemble(x.reshape(1), local, blocks)
    other = lax.ppermute(mine, "sp_1", [(0, 1), (1, 0)])
    back = lax.all_to_all(local, SP, 0, 0, tiled=True)
    return project(core.reshape(1), back, mine, other).T[None]


def solution(mesh):
    split = Mesh(mesh.devices.reshape(8, 2, 12, 4), ("sp_0", "sp_1", "z", "x"))
    dp = ("z", "x")
    return jax.shard_map(
        body,
        mesh=split,
        in_specs=(P(dp, SP, None), P(dp, SP, None), P(dp, SP, None), P(dp, SP, None), P(None, dp)),
        out_specs=P(dp, SP, None),
        check_vma=False,
    )
```

```python
import math

import jax
import jax.numpy as jnp
from jax import lax
from jax.experimental import pallas as pl
from jax.experimental.pallas import tpu as pltpu
from jax.sharding import Mesh
from jax.sharding import PartitionSpec as P


SP = ("sp_0", "sp_1")
LOG2E = math.log2(math.e)
VMEM = pl.BlockSpec(memory_space=pltpu.VMEM)
SMEM = pl.BlockSpec(memory_space=pltpu.SMEM)
HBM = pl.BlockSpec(memory_space=pltpu.HBM)


def swap_halves(a):
    return jnp.concatenate([a[:, 64:], a[:, :64]], axis=1)


def low_lanes(shape):
    return lax.broadcasted_iota(jnp.int32, shape, 1) < 64


def interleave(first, second):
    lanes = low_lanes(first.shape)
    return (
        jnp.where(lanes, first, swap_halves(second)),
        jnp.where(lanes, swap_halves(first), second),
    )


def pack_kernel(queries, keys, values, out, taken, packed, arrived, left):
    heads = out.shape[0]
    groups = arrived.shape[0]
    width, each = taken.shape[2] // groups, heads // groups

    def arrival(g, t):
        columns = slice(width * g, width * g + width)
        source = (queries, keys, values)[t]
        return pltpu.make_async_copy(
            source.at[:, columns], taken.at[t, :, columns], arrived.at[g, t]
        )

    def departure(g):
        block = slice(each * g, each * g + each)
        return pltpu.make_async_copy(packed.at[block], out.at[block], left.at[g])

    for g in range(groups):
        for t in range(3):
            arrival(g, t).start()
    for g in range(groups):
        for t in range(3):
            arrival(g, t).wait()
            for j in range(each * g // 2, (each * g + each) // 2):
                columns = slice(128 * j, 128 * j + 128)
                packed[2 * j, t], packed[2 * j + 1, t] = interleave(
                    taken[t, 0:128, columns], taken[t, 128:256, columns]
                )
        departure(g).start()
    for g in range(groups):
        departure(g).wait()


def pack(queries, keys, values):
    rows, width = queries.shape
    heads, groups = width // 64, 4
    return pl.pallas_call(
        pack_kernel,
        out_shape=jax.ShapeDtypeStruct((heads, 3, rows // 2, 128), jnp.bfloat16),
        in_specs=[HBM] * 3,
        out_specs=HBM,
        scratch_shapes=[
            pltpu.VMEM((3, rows, width), jnp.bfloat16),
            pltpu.VMEM((heads, 3, rows // 2, 128), jnp.bfloat16),
            pltpu.SemaphoreType.DMA((groups, 3)),
            pltpu.SemaphoreType.DMA((groups,)),
        ],
        compiler_params=pltpu.CompilerParams(vmem_limit_bytes=60 * 2**20),
        cost_estimate=pl.CostEstimate(flops=1_000_000, bytes_accessed=3_000_000, transcendentals=0),
        name="pack",
    )(queries, keys, values)


def gate_kernel(gate, out):
    row = lax.broadcasted_iota(jnp.int32, (8, 128), 0)
    for n in range(gate.shape[0]):
        g = jnp.broadcast_to(gate[n : n + 1, :] * -LOG2E, (8, 128))
        high = g.astype(jnp.bfloat16).astype(jnp.float32)
        rest = g - high
        middle = rest.astype(jnp.bfloat16).astype(jnp.float32)
        low = rest - middle
        rows = jnp.where(row == 0, high, jnp.where(row == 1, middle, jnp.where(row == 2, low, 0.0)))
        tile = jnp.concatenate(
            [jnp.zeros((64, 128), jnp.float32), rows, jnp.zeros((56, 128), jnp.float32)], axis=0
        )
        out[128 * n : 128 * n + 128, :] = tile.T.astype(jnp.bfloat16)


def gate_columns(gate):
    return pl.pallas_call(
        gate_kernel,
        out_shape=jax.ShapeDtypeStruct((gate.size, 128), jnp.bfloat16),
        in_specs=[VMEM],
        out_specs=VMEM,
        cost_estimate=pl.CostEstimate(flops=10_000_000, bytes_accessed=1_000_000, transcendentals=0),
        compiler_params=pltpu.CompilerParams(vmem_limit_bytes=6 * 2**20),
        name="gate_columns",
    )(gate)


def attend_kernel(parts, gate, out, keys, values, logits):
    count = parts.shape[0]
    lanes = low_lanes((128, 128))
    values[64:80, :] = jnp.ones((16, values.shape[1]), jnp.bfloat16)
    for b in range(count):
        base = 256 * b
        k = parts[b, 1]
        swapped = swap_halves(k)
        keys[base : base + 128, 0:128] = jnp.where(lanes, k, swapped)
        keys[base + 128 : base + 256, 0:128] = jnp.where(lanes, swapped, k)
        keys[base : base + 128, 128:256] = jnp.where(lanes, k, gate[base : base + 128, :])
        keys[base + 128 : base + 256, 128:256] = jnp.where(
            lanes, swapped, gate[base + 128 : base + 256, :]
        )
        v = parts[b, 2].T
        values[0:64, base : base + 128] = v[:64]
        values[0:64, base + 128 : base + 256] = v[64:]
    causal = lax.broadcasted_iota(jnp.int32, (256, 256), 0) <= lax.broadcasted_iota(
        jnp.int32, (256, 256), 1
    )

    def first(i):
        q = parts[i, 0].astype(jnp.float32).T
        q = jnp.concatenate([q[:64], q[64:]], axis=1) * (LOG2E / 8.0)
        high = q.astype(jnp.bfloat16)
        rest = q - high.astype(jnp.float32)
        middle = rest.astype(jnp.bfloat16)
        low = (rest - middle.astype(jnp.float32)).astype(jnp.bfloat16)
        queries = jnp.concatenate([high, middle, low, jnp.ones((64, 256), jnp.bfloat16)], axis=0)
        peak = None
        for j in range(i + 1):
            s = jnp.dot(
                keys[256 * j : 256 * j + 256, :], queries, preferred_element_type=jnp.float32
            )
            if j == i:
                s = jnp.where(causal, s, -jnp.inf)
            logits[i % 2, 256 * j : 256 * j + 256, :] = s
            top = jnp.max(s.reshape(32, 8, 256), axis=0)
            peak = top if peak is None else jnp.maximum(peak, top)
        return jnp.max(peak, axis=0, keepdims=True)

    def second(i, peak):
        total = None
        for j in range(i + 1):
            p = jnp.exp2(logits[i % 2, 256 * j : 256 * j + 256, :] - peak).astype(jnp.bfloat16)
            o = jnp.dot(
                values[:, 256 * j : 256 * j + 256], p, preferred_element_type=jnp.float32
            )
            total = o if total is None else total + o
        out[i] = (total[:64] / total[64:65]).astype(jnp.bfloat16)

    peak = first(0)
    for i in range(count):
        following = first(i + 1) if i + 1 < count else None
        second(i, peak)
        peak = following


def attend(parts, gate):
    count = parts.shape[0]
    length = 256 * count
    return pl.pallas_call(
        attend_kernel,
        out_shape=jax.ShapeDtypeStruct((count, 64, 256), jnp.bfloat16),
        in_specs=[VMEM] * 2,
        out_specs=VMEM,
        scratch_shapes=[
            pltpu.VMEM((length, 256), jnp.bfloat16),
            pltpu.VMEM((80, length), jnp.bfloat16),
            pltpu.VMEM((2, length, 256), jnp.float32),
        ],
        compiler_params=pltpu.CompilerParams(vmem_limit_bytes=32 * 2**20),
        cost_estimate=pl.CostEstimate(
            flops=10_000_000_000, bytes_accessed=4_000_000, transcendentals=9_000_000
        ),
        name="attend",
    )(parts, gate)


def assemble_kernel(me, after, *refs):
    del after
    *blocks, out = refs
    hops = len(blocks)
    groups, columns, _ = blocks[0].shape
    for k in range(hops):
        for hop in range(hops):

            @pl.when(lax.rem(me[0] - k + hops, hops) == hop)
            def _():
                @pl.loop(0, groups)
                def _(z):
                    first = pl.multiple_of(hops * columns * z, 8)
                    group = out.at[pl.ds(first, hops * columns)]
                    group[columns * k : columns * k + columns, :] = blocks[hop][z]


def assemble(me, after, blocks):
    groups, columns, depth = blocks[0].shape
    return pl.pallas_call(
        assemble_kernel,
        out_shape=jax.ShapeDtypeStruct((len(blocks) * groups * columns, depth), jnp.bfloat16),
        in_specs=[SMEM, pl.BlockSpec(memory_space=pl.ANY)] + [VMEM] * len(blocks),
        out_specs=VMEM,
        compiler_params=pltpu.CompilerParams(vmem_limit_bytes=16 * 2**20),
        cost_estimate=pl.CostEstimate(flops=1_000_000, bytes_accessed=4_300_000, transcendentals=0),
        name="assemble",
    )(me, after, *blocks)


def project_kernel(core, attended, mine, other, out):
    heads, depth, rows = attended.shape
    c, half = core[0], heads // 2

    def columns(first):
        return attended[pl.ds(first, half)].reshape(half * depth, rows)

    total = jnp.dot(mine[...], columns(c * half), preferred_element_type=jnp.float32)
    total += jnp.dot(other[...], columns((1 - c) * half), preferred_element_type=jnp.float32)
    out[...] = total.astype(jnp.bfloat16)


def project(core, attended, mine, other):
    columns, step = mine.shape[0], 352
    return pl.pallas_call(
        project_kernel,
        out_shape=jax.ShapeDtypeStruct((columns, attended.shape[2]), jnp.bfloat16),
        grid=(columns // step,),
        in_specs=[
            SMEM,
            pl.BlockSpec(attended.shape, lambda i: (0, 0, 0)),
            pl.BlockSpec((step, mine.shape[1]), lambda i: (i, 0)),
            pl.BlockSpec((step, other.shape[1]), lambda i: (i, 0)),
        ],
        out_specs=pl.BlockSpec((step, attended.shape[2]), lambda i: (i, 0)),
        compiler_params=pltpu.CompilerParams(vmem_limit_bytes=16 * 2**20),
        cost_estimate=pl.CostEstimate(
            flops=1_100_000_000, bytes_accessed=6_000_000, transcendentals=0
        ),
        name="project",
    )(core, attended, mine, other)


def body(queries, keys, values, cum_gate, out_weight):
    core, x = lax.axis_index("sp_1"), lax.axis_index("x")
    packed = pack(queries[0], keys[0], values[0])
    parts = lax.all_to_all(packed, SP, 0, 0, tiled=True)
    gate = gate_columns(cum_gate[0, 0].reshape(-1, 128))

    depth = out_weight.shape[0] // 2
    own = lax.dynamic_slice_in_dim(out_weight.T, core * depth, depth, axis=1)
    along_z = lax.all_gather(own[None], "z", axis=0, tiled=True)
    n = lax.axis_size("x")
    blocks = [along_z] + [
        lax.ppermute(along_z, "x", [(i, (i + hop) % n) for i in range(n)])
        for hop in range(1, n)
    ]
    local = attend(parts, gate)
    mine = assemble(x.reshape(1), local, blocks)
    other = lax.ppermute(mine, "sp_1", [(0, 1), (1, 0)])
    back = lax.all_to_all(local, SP, 0, 0, tiled=True)
    return project(core.reshape(1), back, mine, other).T[None]


def solution(mesh):
    split = Mesh(mesh.devices.reshape(8, 2, 12, 4), ("sp_0", "sp_1", "z", "x"))
    dp = ("z", "x")
    return jax.shard_map(
        body,
        mesh=split,
        in_specs=(P(dp, SP, None), P(dp, SP, None), P(dp, SP, None), P(dp, SP, None), P(None, dp)),
        out_specs=P(dp, SP, None),
        check_vma=False,
    )
```

```python
import math

import jax
import jax.numpy as jnp
from jax import lax
from jax.experimental import pallas as pl
from jax.experimental.pallas import tpu as pltpu
from jax.sharding import Mesh
from jax.sharding import PartitionSpec as P


SP = ("sp_0", "sp_1")
LOG2E = math.log2(math.e)
VMEM = pl.BlockSpec(memory_space=pltpu.VMEM)
SMEM = pl.BlockSpec(memory_space=pltpu.SMEM)
HBM = pl.BlockSpec(memory_space=pltpu.HBM)


def swap_halves(a):
    return jnp.concatenate([a[:, 64:], a[:, :64]], axis=1)


def low_lanes(shape):
    return lax.broadcasted_iota(jnp.int32, shape, 1) < 64


def interleave(first, second):
    lanes = low_lanes(first.shape)
    return (
        jnp.where(lanes, first, swap_halves(second)),
        jnp.where(lanes, swap_halves(first), second),
    )


def pack_kernel(queries, keys, values, out, taken, packed, arrived, left):
    heads = out.shape[0]
    groups = arrived.shape[0]
    width, each = taken.shape[2] // groups, heads // groups

    def arrival(g, t):
        columns = slice(width * g, width * g + width)
        source = (queries, keys, values)[t]
        return pltpu.make_async_copy(
            source.at[:, columns], taken.at[t, :, columns], arrived.at[g, t]
        )

    def departure(g):
        block = slice(each * g, each * g + each)
        return pltpu.make_async_copy(packed.at[block], out.at[block], left.at[g])

    for g in range(groups):
        for t in range(3):
            arrival(g, t).start()
    for g in range(groups):
        for t in range(3):
            arrival(g, t).wait()
            for j in range(each * g // 2, (each * g + each) // 2):
                columns = slice(128 * j, 128 * j + 128)
                packed[2 * j, t], packed[2 * j + 1, t] = interleave(
                    taken[t, 0:128, columns], taken[t, 128:256, columns]
                )
        departure(g).start()
    for g in range(groups):
        departure(g).wait()


def pack(queries, keys, values):
    rows, width = queries.shape
    heads, groups = width // 64, 4
    return pl.pallas_call(
        pack_kernel,
        out_shape=jax.ShapeDtypeStruct((heads, 3, rows // 2, 128), jnp.bfloat16),
        in_specs=[HBM] * 3,
        out_specs=HBM,
        scratch_shapes=[
            pltpu.VMEM((3, rows, width), jnp.bfloat16),
            pltpu.VMEM((heads, 3, rows // 2, 128), jnp.bfloat16),
            pltpu.SemaphoreType.DMA((groups, 3)),
            pltpu.SemaphoreType.DMA((groups,)),
        ],
        compiler_params=pltpu.CompilerParams(vmem_limit_bytes=60 * 2**20),
        cost_estimate=pl.CostEstimate(flops=1_000_000, bytes_accessed=3_000_000, transcendentals=0),
        name="pack",
    )(queries, keys, values)


def gate_kernel(gate, out):
    row = lax.broadcasted_iota(jnp.int32, (8, 128), 0)
    for n in range(gate.shape[0]):
        g = jnp.broadcast_to(gate[n : n + 1, :] * -LOG2E, (8, 128))
        high = g.astype(jnp.bfloat16).astype(jnp.float32)
        rest = g - high
        middle = rest.astype(jnp.bfloat16).astype(jnp.float32)
        low = rest - middle
        rows = jnp.where(row == 0, high, jnp.where(row == 1, middle, jnp.where(row == 2, low, 0.0)))
        tile = jnp.concatenate(
            [jnp.zeros((64, 128), jnp.float32), rows, jnp.zeros((56, 128), jnp.float32)], axis=0
        )
        out[128 * n : 128 * n + 128, :] = tile.T.astype(jnp.bfloat16)


def gate_columns(gate):
    return pl.pallas_call(
        gate_kernel,
        out_shape=jax.ShapeDtypeStruct((gate.size, 128), jnp.bfloat16),
        in_specs=[VMEM],
        out_specs=VMEM,
        cost_estimate=pl.CostEstimate(flops=10_000_000, bytes_accessed=1_000_000, transcendentals=0),
        compiler_params=pltpu.CompilerParams(vmem_limit_bytes=6 * 2**20),
        name="gate_columns",
    )(gate)


def attend_kernel(parts, gate, out, keys, values, logits):
    count = parts.shape[0]
    lanes = low_lanes((128, 128))
    values[64:80, :] = jnp.ones((16, values.shape[1]), jnp.bfloat16)
    for b in range(count):
        base = 256 * b
        k = parts[b, 1]
        swapped = swap_halves(k)
        keys[base : base + 128, 0:128] = jnp.where(lanes, k, swapped)
        keys[base + 128 : base + 256, 0:128] = jnp.where(lanes, swapped, k)
        keys[base : base + 128, 128:256] = jnp.where(lanes, k, gate[base : base + 128, :])
        keys[base + 128 : base + 256, 128:256] = jnp.where(
            lanes, swapped, gate[base + 128 : base + 256, :]
        )
        v = parts[b, 2].T
        values[0:64, base : base + 128] = v[:64]
        values[0:64, base + 128 : base + 256] = v[64:]
    causal = lax.broadcasted_iota(jnp.int32, (256, 256), 0) <= lax.broadcasted_iota(
        jnp.int32, (256, 256), 1
    )

    def first(i):
        q = parts[i, 0].astype(jnp.float32).T
        q = jnp.concatenate([q[:64], q[64:]], axis=1) * (LOG2E / 8.0)
        high = q.astype(jnp.bfloat16)
        rest = q - high.astype(jnp.float32)
        middle = rest.astype(jnp.bfloat16)
        low = (rest - middle.astype(jnp.float32)).astype(jnp.bfloat16)
        queries = jnp.concatenate([high, middle, low, jnp.ones((64, 256), jnp.bfloat16)], axis=0)
        peak = None
        for j in range(i + 1):
            s = jnp.dot(
                keys[256 * j : 256 * j + 256, :], queries, preferred_element_type=jnp.float32
            )
            if j == i:
                s = jnp.where(causal, s, -jnp.inf)
            logits[i % 2, 256 * j : 256 * j + 256, :] = s
            top = jnp.max(s.reshape(32, 8, 256), axis=0)
            peak = top if peak is None else jnp.maximum(peak, top)
        return jnp.max(peak, axis=0, keepdims=True)

    def second(i, peak):
        total = None
        for j in range(i + 1):
            p = jnp.exp2(logits[i % 2, 256 * j : 256 * j + 256, :] - peak).astype(jnp.bfloat16)
            o = jnp.dot(
                values[:, 256 * j : 256 * j + 256], p, preferred_element_type=jnp.float32
            )
            total = o if total is None else total + o
        out[i] = (total[:64] / total[64:65]).astype(jnp.bfloat16)

    peak = first(0)
    for i in range(count):
        following = first(i + 1) if i + 1 < count else None
        second(i, peak)
        peak = following


def attend(parts, gate):
    count = parts.shape[0]
    length = 256 * count
    return pl.pallas_call(
        attend_kernel,
        out_shape=jax.ShapeDtypeStruct((count, 64, 256), jnp.bfloat16),
        in_specs=[VMEM] * 2,
        out_specs=VMEM,
        scratch_shapes=[
            pltpu.VMEM((length, 256), jnp.bfloat16),
            pltpu.VMEM((80, length), jnp.bfloat16),
            pltpu.VMEM((2, length, 256), jnp.float32),
        ],
        compiler_params=pltpu.CompilerParams(vmem_limit_bytes=32 * 2**20),
        cost_estimate=pl.CostEstimate(
            flops=10_000_000_000, bytes_accessed=4_000_000, transcendentals=9_000_000
        ),
        name="attend",
    )(parts, gate)


def assemble_kernel(me, after, *refs):
    del after
    *blocks, out = refs
    hops = len(blocks)
    groups, columns, _ = blocks[0].shape
    for k in range(hops):
        for hop in range(hops):

            @pl.when(lax.rem(me[0] - k + hops, hops) == hop)
            def _():
                @pl.loop(0, groups)
                def _(z):
                    first = pl.multiple_of(hops * columns * z, 8)
                    group = out.at[pl.ds(first, hops * columns)]
                    group[columns * k : columns * k + columns, :] = blocks[hop][z]


def assemble(me, after, blocks):
    groups, columns, depth = blocks[0].shape
    return pl.pallas_call(
        assemble_kernel,
        out_shape=jax.ShapeDtypeStruct((len(blocks) * groups * columns, depth), jnp.bfloat16),
        in_specs=[SMEM, pl.BlockSpec(memory_space=pl.ANY)] + [VMEM] * len(blocks),
        out_specs=VMEM,
        compiler_params=pltpu.CompilerParams(vmem_limit_bytes=60 * 2**20),
        cost_estimate=pl.CostEstimate(flops=1_000_000, bytes_accessed=4_300_000, transcendentals=0),
        name="assemble",
    )(me, after, *blocks)


def settle_kernel(source, out):
    del source, out


def settle(a):
    return pl.pallas_call(
        settle_kernel,
        out_shape=jax.ShapeDtypeStruct(a.shape, a.dtype),
        in_specs=[HBM],
        out_specs=HBM,
        input_output_aliases={0: 0},
        compiler_params=pltpu.CompilerParams(vmem_limit_bytes=60 * 2**20),
        cost_estimate=pl.CostEstimate(flops=1_000_000, bytes_accessed=8_600_000, transcendentals=0),
        name="settle",
    )(a)


def project_kernel(core, back, mine, other, out, attended, weight, finished, arrived, left):
    heads, depth, rows = attended.shape
    c, half = core[0], heads // 2
    steps = left.shape[0]
    step = out.shape[0] // steps

    def block(n):
        return slice(step * n, step * n + step)

    def arrival(n):
        return [
            pltpu.make_async_copy(source.at[block(n)], weight.at[k, block(n)], arrived.at[n, k])
            for k, source in enumerate((mine, other))
        ]

    def departure(n):
        return pltpu.make_async_copy(finished.at[block(n)], out.at[block(n)], left.at[n])

    whole = pltpu.make_async_copy(back, attended, arrived.at[steps, 0])
    whole.start()
    for n in range(steps):
        for copy in arrival(n):
            copy.start()
    whole.wait()
    halves = [
        attended[pl.ds(first, half)].reshape(half * depth, rows)
        for first in (c * half, (1 - c) * half)
    ]
    for n in range(steps):
        total = None
        for k, copy in enumerate(arrival(n)):
            copy.wait()
            part = jnp.dot(weight[k, block(n), :], halves[k], preferred_element_type=jnp.float32)
            total = part if total is None else total + part
        finished[block(n), :] = total.astype(jnp.bfloat16)
        departure(n).start()
    for n in range(steps):
        departure(n).wait()


def project(core, back, mine, other):
    columns, depth = mine.shape
    rows, steps = back.shape[2], 6
    return pl.pallas_call(
        project_kernel,
        out_shape=jax.ShapeDtypeStruct((columns, rows), jnp.bfloat16),
        in_specs=[SMEM] + [HBM] * 3,
        out_specs=HBM,
        scratch_shapes=[
            pltpu.VMEM(back.shape, jnp.bfloat16),
            pltpu.VMEM((2, columns, depth), jnp.bfloat16),
            pltpu.VMEM((columns, rows), jnp.bfloat16),
            pltpu.SemaphoreType.DMA((steps + 1, 2)),
            pltpu.SemaphoreType.DMA((steps,)),
        ],
        compiler_params=pltpu.CompilerParams(vmem_limit_bytes=60 * 2**20),
        cost_estimate=pl.CostEstimate(
            flops=1_100_000_000, bytes_accessed=6_000_000, transcendentals=0
        ),
        name="project",
    )(core, back, mine, other)


def body(queries, keys, values, cum_gate, out_weight):
    core, x = lax.axis_index("sp_1"), lax.axis_index("x")
    packed = pack(queries[0], keys[0], values[0])
    parts = lax.all_to_all(packed, SP, 0, 0, tiled=True)
    gate = gate_columns(cum_gate[0, 0].reshape(-1, 128))

    depth = out_weight.shape[0] // 2
    own = lax.dynamic_slice_in_dim(out_weight.T, core * depth, depth, axis=1)
    along_z = lax.all_gather(own[None], "z", axis=0, tiled=True)
    n = lax.axis_size("x")
    blocks = [along_z] + [
        lax.ppermute(along_z, "x", [(i, (i + hop) % n) for i in range(n)])
        for hop in range(1, n)
    ]
    local = attend(parts, gate)
    mine = assemble(x.reshape(1), local, blocks)
    other = lax.ppermute(mine, "sp_1", [(0, 1), (1, 0)])
    other = settle(other)
    back = lax.all_to_all(local, SP, 0, 0, tiled=True)
    return project(core.reshape(1), back, mine, other).T[None]


def solution(mesh):
    split = Mesh(mesh.devices.reshape(8, 2, 12, 4), ("sp_0", "sp_1", "z", "x"))
    dp = ("z", "x")
    return jax.shard_map(
        body,
        mesh=split,
        in_specs=(P(dp, SP, None), P(dp, SP, None), P(dp, SP, None), P(dp, SP, None), P(None, dp)),
        out_specs=P(dp, SP, None),
        check_vma=False,
    )
```

```python
import math

import jax
import jax.numpy as jnp
from jax import lax
from jax.experimental import pallas as pl
from jax.experimental.pallas import tpu as pltpu
from jax.sharding import Mesh
from jax.sharding import PartitionSpec as P


SP = ("sp_0", "sp_1")
LOG2E = math.log2(math.e)
VMEM = pl.BlockSpec(memory_space=pltpu.VMEM)
SMEM = pl.BlockSpec(memory_space=pltpu.SMEM)
HBM = pl.BlockSpec(memory_space=pltpu.HBM)


def swap_halves(a):
    return jnp.concatenate([a[:, 64:], a[:, :64]], axis=1)


def low_lanes(shape):
    return lax.broadcasted_iota(jnp.int32, shape, 1) < 64


def interleave(first, second):
    lanes = low_lanes(first.shape)
    return (
        jnp.where(lanes, first, swap_halves(second)),
        jnp.where(lanes, swap_halves(first), second),
    )


def pack_kernel(queries, keys, values, out, taken, packed, arrived, left):
    heads = out.shape[0]
    groups = arrived.shape[0]
    width, each = taken.shape[2] // groups, heads // groups

    def arrival(g, t):
        columns = slice(width * g, width * g + width)
        source = (queries, keys, values)[t]
        return pltpu.make_async_copy(
            source.at[:, columns], taken.at[t, :, columns], arrived.at[g, t]
        )

    def departure(g):
        block = slice(each * g, each * g + each)
        return pltpu.make_async_copy(packed.at[block], out.at[block], left.at[g])

    for g in range(groups):
        for t in range(3):
            arrival(g, t).start()
    for g in range(groups):
        for t in range(3):
            arrival(g, t).wait()
            for j in range(each * g // 2, (each * g + each) // 2):
                columns = slice(128 * j, 128 * j + 128)
                packed[2 * j, t], packed[2 * j + 1, t] = interleave(
                    taken[t, 0:128, columns], taken[t, 128:256, columns]
                )
        departure(g).start()
    for g in range(groups):
        departure(g).wait()


def pack(queries, keys, values):
    rows, width = queries.shape
    heads, groups = width // 64, 4
    return pl.pallas_call(
        pack_kernel,
        out_shape=jax.ShapeDtypeStruct((heads, 3, rows // 2, 128), jnp.bfloat16),
        in_specs=[HBM] * 3,
        out_specs=HBM,
        scratch_shapes=[
            pltpu.VMEM((3, rows, width), jnp.bfloat16),
            pltpu.VMEM((heads, 3, rows // 2, 128), jnp.bfloat16),
            pltpu.SemaphoreType.DMA((groups, 3)),
            pltpu.SemaphoreType.DMA((groups,)),
        ],
        compiler_params=pltpu.CompilerParams(vmem_limit_bytes=60 * 2**20),
        cost_estimate=pl.CostEstimate(flops=1_000_000, bytes_accessed=3_000_000, transcendentals=0),
        name="pack",
    )(queries, keys, values)


def gate_kernel(gate, out):
    row = lax.broadcasted_iota(jnp.int32, (8, 128), 0)

    def split(n):
        g = jnp.broadcast_to(gate[n : n + 1, :] * -LOG2E, (8, 128))
        high = g.astype(jnp.bfloat16).astype(jnp.float32)
        rest = g - high
        middle = rest.astype(jnp.bfloat16).astype(jnp.float32)
        low = rest - middle
        return jnp.where(row == 0, high, jnp.where(row == 1, middle, jnp.where(row == 2, low, 0.0)))

    empty = jnp.zeros((56, 128), jnp.float32)
    for b in range(gate.shape[0] // 2):
        tile = jnp.concatenate([split(2 * b + 1), empty, split(2 * b), empty], axis=0)
        out[128 * b : 128 * b + 128, :] = tile.T.astype(jnp.bfloat16)


def gate_columns(gate):
    return pl.pallas_call(
        gate_kernel,
        out_shape=jax.ShapeDtypeStruct((gate.size // 2, 128), jnp.bfloat16),
        in_specs=[VMEM],
        out_specs=VMEM,
        compiler_params=pltpu.CompilerParams(vmem_limit_bytes=6 * 2**20),
        cost_estimate=pl.CostEstimate(flops=10_000_000, bytes_accessed=500_000, transcendentals=0),
        name="gate_columns",
    )(gate)


def attend_kernel(parts, gate, out, keys, values, logits):
    count = parts.shape[0]
    lanes = low_lanes((128, 128))
    values[64:80, :] = jnp.ones((16, values.shape[1]), jnp.bfloat16)
    for b in range(count):
        base = 256 * b
        k = parts[b, 1]
        swapped = swap_halves(k)
        keys[base : base + 128, 0:128] = jnp.where(lanes, k, swapped)
        keys[base + 128 : base + 256, 0:128] = jnp.where(lanes, swapped, k)
        g = gate[128 * b : 128 * b + 128, :]
        keys[base : base + 128, 128:256] = jnp.where(lanes, k, g)
        keys[base + 128 : base + 256, 128:256] = jnp.where(lanes, swapped, swap_halves(g))
        v = parts[b, 2].T
        values[0:64, base : base + 128] = v[:64]
        values[0:64, base + 128 : base + 256] = v[64:]
    causal = lax.broadcasted_iota(jnp.int32, (256, 256), 0) <= lax.broadcasted_iota(
        jnp.int32, (256, 256), 1
    )

    def first(i):
        q = parts[i, 0].astype(jnp.float32).T
        q = jnp.concatenate([q[:64], q[64:]], axis=1) * (LOG2E / 8.0)
        high = q.astype(jnp.bfloat16)
        rest = q - high.astype(jnp.float32)
        middle = rest.astype(jnp.bfloat16)
        low = (rest - middle.astype(jnp.float32)).astype(jnp.bfloat16)
        queries = jnp.concatenate([high, middle, low, jnp.ones((64, 256), jnp.bfloat16)], axis=0)
        peak = None
        for j in range(i + 1):
            s = jnp.dot(
                keys[256 * j : 256 * j + 256, :], queries, preferred_element_type=jnp.float32
            )
            if j == i:
                s = jnp.where(causal, s, -jnp.inf)
            logits[i % 2, 256 * j : 256 * j + 256, :] = s
            top = jnp.max(s.reshape(32, 8, 256), axis=0)
            peak = top if peak is None else jnp.maximum(peak, top)
        return jnp.max(peak, axis=0, keepdims=True)

    def second(i, peak):
        total = None
        for j in range(i + 1):
            p = jnp.exp2(logits[i % 2, 256 * j : 256 * j + 256, :] - peak).astype(jnp.bfloat16)
            o = jnp.dot(
                values[:, 256 * j : 256 * j + 256], p, preferred_element_type=jnp.float32
            )
            total = o if total is None else total + o
        out[i] = (total[:64] / total[64:65]).astype(jnp.bfloat16)

    peak = first(0)
    for i in range(count):
        following = first(i + 1) if i + 1 < count else None
        second(i, peak)
        peak = following


def attend(parts, gate):
    count = parts.shape[0]
    length = 256 * count
    return pl.pallas_call(
        attend_kernel,
        out_shape=jax.ShapeDtypeStruct((count, 64, 256), jnp.bfloat16),
        in_specs=[VMEM] * 2,
        out_specs=VMEM,
        scratch_shapes=[
            pltpu.VMEM((length, 256), jnp.bfloat16),
            pltpu.VMEM((80, length), jnp.bfloat16),
            pltpu.VMEM((2, length, 256), jnp.float32),
        ],
        compiler_params=pltpu.CompilerParams(vmem_limit_bytes=32 * 2**20),
        cost_estimate=pl.CostEstimate(
            flops=10_000_000_000, bytes_accessed=4_000_000, transcendentals=9_000_000
        ),
        name="attend",
    )(parts, gate)


def assemble_kernel(me, after, *refs):
    del after
    *blocks, out = refs
    hops = len(blocks)
    groups, columns, _ = blocks[0].shape
    for k in range(hops):
        for hop in range(hops):

            @pl.when(lax.rem(me[0] - k + hops, hops) == hop)
            def _():
                @pl.loop(0, groups)
                def _(z):
                    first = pl.multiple_of(hops * columns * z, 8)
                    group = out.at[pl.ds(first, hops * columns)]
                    group[columns * k : columns * k + columns, :] = blocks[hop][z]


def assemble(me, after, blocks):
    groups, columns, depth = blocks[0].shape
    return pl.pallas_call(
        assemble_kernel,
        out_shape=jax.ShapeDtypeStruct((len(blocks) * groups * columns, depth), jnp.bfloat16),
        in_specs=[SMEM, pl.BlockSpec(memory_space=pl.ANY)] + [VMEM] * len(blocks),
        out_specs=VMEM,
        compiler_params=pltpu.CompilerParams(vmem_limit_bytes=16 * 2**20),
        cost_estimate=pl.CostEstimate(flops=1_000_000, bytes_accessed=4_300_000, transcendentals=0),
        name="assemble",
    )(me, after, *blocks)


def project_kernel(core, attended, mine, source, out, other, partial, finished, arrived, left):
    heads, depth, rows = attended.shape
    c, half = core[0], heads // 2
    steps = left.shape[0]
    step = out.shape[0] // steps

    def block(n):
        return slice(step * n, step * n + step)

    def columns(first):
        return attended[pl.ds(first, half)].reshape(half * depth, rows)

    def departure(n):
        return pltpu.make_async_copy(finished.at[block(n)], out.at[block(n)], left.at[n])

    arrival = pltpu.make_async_copy(source, other, arrived)
    arrival.start()
    partial[...] = jnp.dot(mine[...], columns(c * half), preferred_element_type=jnp.float32)
    arrival.wait()
    rest = columns((1 - c) * half)
    for n in range(steps):
        total = partial[block(n), :] + jnp.dot(
            other[block(n), :], rest, preferred_element_type=jnp.float32
        )
        finished[block(n), :] = total.astype(jnp.bfloat16)
        departure(n).start()
    for n in range(steps):
        departure(n).wait()


def project(core, attended, mine, other):
    columns, depth = mine.shape
    rows, steps = attended.shape[2], 3
    return pl.pallas_call(
        project_kernel,
        out_shape=jax.ShapeDtypeStruct((columns, rows), jnp.bfloat16),
        in_specs=[SMEM, VMEM, VMEM, HBM],
        out_specs=HBM,
        scratch_shapes=[
            pltpu.VMEM((columns, depth), jnp.bfloat16),
            pltpu.VMEM((columns, rows), jnp.float32),
            pltpu.VMEM((columns, rows), jnp.bfloat16),
            pltpu.SemaphoreType.DMA,
            pltpu.SemaphoreType.DMA((steps,)),
        ],
        compiler_params=pltpu.CompilerParams(vmem_limit_bytes=16 * 2**20),
        cost_estimate=pl.CostEstimate(
            flops=1_100_000_000, bytes_accessed=6_000_000, transcendentals=0
        ),
        name="project",
    )(core, attended, mine, other)


def body(queries, keys, values, cum_gate, out_weight):
    core, x = lax.axis_index("sp_1"), lax.axis_index("x")
    packed = pack(queries[0], keys[0], values[0])
    parts = lax.all_to_all(packed, SP, 0, 0, tiled=True)
    gate = gate_columns(cum_gate[0, 0].reshape(-1, 128))

    depth = out_weight.shape[0] // 2
    own = lax.dynamic_slice_in_dim(out_weight.T, core * depth, depth, axis=1)
    along_z = lax.all_gather(own[None], "z", axis=0, tiled=True)
    n = lax.axis_size("x")
    blocks = [along_z] + [
        lax.ppermute(along_z, "x", [(i, (i + hop) % n) for i in range(n)])
        for hop in range(1, n)
    ]
    local = attend(parts, gate)
    mine = assemble(x.reshape(1), local, blocks)
    other = lax.ppermute(mine, "sp_1", [(0, 1), (1, 0)])
    back = lax.all_to_all(local, SP, 0, 0, tiled=True)
    return project(core.reshape(1), back, mine, other).T[None]


def solution(mesh):
    split = Mesh(mesh.devices.reshape(8, 2, 12, 4), ("sp_0", "sp_1", "z", "x"))
    dp = ("z", "x")
    return jax.shard_map(
        body,
        mesh=split,
        in_specs=(P(dp, SP, None), P(dp, SP, None), P(dp, SP, None), P(dp, SP, None), P(None, dp)),
        out_specs=P(dp, SP, None),
        check_vma=False,
    )
```

```python
import math

import jax
import jax.numpy as jnp
from jax import lax
from jax.experimental import pallas as pl
from jax.experimental.pallas import tpu as pltpu
from jax.sharding import Mesh
from jax.sharding import PartitionSpec as P


SP = ("sp_0", "sp_1")
LOG2E = math.log2(math.e)
VMEM = pl.BlockSpec(memory_space=pltpu.VMEM)
SMEM = pl.BlockSpec(memory_space=pltpu.SMEM)
HBM = pl.BlockSpec(memory_space=pltpu.HBM)


def swap_halves(a):
    return jnp.concatenate([a[:, 64:], a[:, :64]], axis=1)


def low_lanes(shape):
    return lax.broadcasted_iota(jnp.int32, shape, 1) < 64


def interleave(first, second):
    lanes = low_lanes(first.shape)
    return (
        jnp.where(lanes, first, swap_halves(second)),
        jnp.where(lanes, swap_halves(first), second),
    )


def pack_kernel(queries, keys, values, out, taken, packed, arrived, left):
    heads = out.shape[0]
    groups = arrived.shape[0]
    width, each = taken.shape[2] // groups, heads // groups

    def arrival(g, t):
        columns = slice(width * g, width * g + width)
        source = (queries, keys, values)[t]
        return pltpu.make_async_copy(
            source.at[:, columns], taken.at[t, :, columns], arrived.at[g, t]
        )

    def departure(g):
        block = slice(each * g, each * g + each)
        return pltpu.make_async_copy(packed.at[block], out.at[block], left.at[g])

    for g in range(groups):
        for t in range(3):
            arrival(g, t).start()
    for g in range(groups):
        for t in range(3):
            arrival(g, t).wait()
            for j in range(each * g // 2, (each * g + each) // 2):
                columns = slice(128 * j, 128 * j + 128)
                packed[2 * j, t], packed[2 * j + 1, t] = interleave(
                    taken[t, 0:128, columns], taken[t, 128:256, columns]
                )
        departure(g).start()
    for g in range(groups):
        departure(g).wait()


def pack(queries, keys, values):
    rows, width = queries.shape
    heads, groups = width // 64, 4
    return pl.pallas_call(
        pack_kernel,
        out_shape=jax.ShapeDtypeStruct((heads, 3, rows // 2, 128), jnp.bfloat16),
        in_specs=[HBM] * 3,
        out_specs=HBM,
        scratch_shapes=[
            pltpu.VMEM((3, rows, width), jnp.bfloat16),
            pltpu.VMEM((heads, 3, rows // 2, 128), jnp.bfloat16),
            pltpu.SemaphoreType.DMA((groups, 3)),
            pltpu.SemaphoreType.DMA((groups,)),
        ],
        compiler_params=pltpu.CompilerParams(vmem_limit_bytes=60 * 2**20),
        cost_estimate=pl.CostEstimate(flops=1_000_000, bytes_accessed=3_000_000, transcendentals=0),
        name="pack",
    )(queries, keys, values)


def gate_kernel(gate, out):
    row = lax.broadcasted_iota(jnp.int32, (8, 128), 0)

    def split(n):
        g = jnp.broadcast_to(gate[n : n + 1, :] * -LOG2E, (8, 128))
        high = g.astype(jnp.bfloat16).astype(jnp.float32)
        rest = g - high
        middle = rest.astype(jnp.bfloat16).astype(jnp.float32)
        low = rest - middle
        return jnp.where(row == 0, high, jnp.where(row == 1, middle, jnp.where(row == 2, low, 0.0)))

    empty = jnp.zeros((56, 128), jnp.float32)
    for b in range(gate.shape[0] // 2):
        tile = jnp.concatenate([split(2 * b + 1), empty, split(2 * b), empty], axis=0)
        out[128 * b : 128 * b + 128, :] = tile.T.astype(jnp.bfloat16)


def gate_columns(gate):
    return pl.pallas_call(
        gate_kernel,
        out_shape=jax.ShapeDtypeStruct((gate.size // 2, 128), jnp.bfloat16),
        in_specs=[VMEM],
        out_specs=VMEM,
        compiler_params=pltpu.CompilerParams(vmem_limit_bytes=6 * 2**20),
        cost_estimate=pl.CostEstimate(flops=10_000_000, bytes_accessed=500_000, transcendentals=0),
        name="gate_columns",
    )(gate)


def attend_kernel(parts, gate, out, keys, values, logits):
    count = parts.shape[0]
    lanes = low_lanes((128, 128))
    values[64:80, :] = jnp.ones((16, values.shape[1]), jnp.bfloat16)
    for b in range(count):
        base = 256 * b
        k = parts[b, 1]
        swapped = swap_halves(k)
        keys[base : base + 128, 0:128] = jnp.where(lanes, k, swapped)
        keys[base + 128 : base + 256, 0:128] = jnp.where(lanes, swapped, k)
        g = gate[128 * b : 128 * b + 128, :]
        keys[base : base + 128, 128:256] = jnp.where(lanes, k, g)
        keys[base + 128 : base + 256, 128:256] = jnp.where(lanes, swapped, swap_halves(g))
        v = parts[b, 2].T
        values[0:64, base : base + 128] = v[:64]
        values[0:64, base + 128 : base + 256] = v[64:]
    causal = lax.broadcasted_iota(jnp.int32, (256, 256), 0) <= lax.broadcasted_iota(
        jnp.int32, (256, 256), 1
    )

    def first(i):
        q = parts[i, 0].astype(jnp.float32).T
        q = jnp.concatenate([q[:64], q[64:]], axis=1) * (LOG2E / 8.0)
        high = q.astype(jnp.bfloat16)
        rest = q - high.astype(jnp.float32)
        middle = rest.astype(jnp.bfloat16)
        low = (rest - middle.astype(jnp.float32)).astype(jnp.bfloat16)
        queries = jnp.concatenate([high, middle, low, jnp.ones((64, 256), jnp.bfloat16)], axis=0)
        peak = None
        for j in range(i + 1):
            s = jnp.dot(
                keys[256 * j : 256 * j + 256, :], queries, preferred_element_type=jnp.float32
            )
            if j == i:
                s = jnp.where(causal, s, -jnp.inf)
            logits[i % 2, 256 * j : 256 * j + 256, :] = s
            top = jnp.max(s.reshape(32, 8, 256), axis=0)
            peak = top if peak is None else jnp.maximum(peak, top)
        return jnp.max(peak, axis=0, keepdims=True)

    def second(i, peak):
        total = None
        for j in range(i + 1):
            p = jnp.exp2(logits[i % 2, 256 * j : 256 * j + 256, :] - peak).astype(jnp.bfloat16)
            o = jnp.dot(
                values[:, 256 * j : 256 * j + 256], p, preferred_element_type=jnp.float32
            )
            total = o if total is None else total + o
        out[i] = (total[:64] / total[64:65]).astype(jnp.bfloat16)

    peak = first(0)
    for i in range(count):
        following = first(i + 1) if i + 1 < count else None
        second(i, peak)
        peak = following


def attend(parts, gate):
    count = parts.shape[0]
    length = 256 * count
    return pl.pallas_call(
        attend_kernel,
        out_shape=jax.ShapeDtypeStruct((count, 64, 256), jnp.bfloat16),
        in_specs=[VMEM] * 2,
        out_specs=VMEM,
        scratch_shapes=[
            pltpu.VMEM((length, 256), jnp.bfloat16),
            pltpu.VMEM((80, length), jnp.bfloat16),
            pltpu.VMEM((2, length, 256), jnp.float32),
        ],
        compiler_params=pltpu.CompilerParams(vmem_limit_bytes=32 * 2**20),
        cost_estimate=pl.CostEstimate(
            flops=10_000_000_000, bytes_accessed=4_000_000, transcendentals=9_000_000
        ),
        name="attend",
    )(parts, gate)


def assemble_kernel(me, after, *refs):
    del after
    *blocks, out = refs
    hops = len(blocks)
    groups, columns, _ = blocks[0].shape
    for k in range(hops):
        for hop in range(hops):

            @pl.when(lax.rem(me[0] - k + hops, hops) == hop)
            def _():
                @pl.loop(0, groups)
                def _(z):
                    first = pl.multiple_of(hops * columns * z, 8)
                    group = out.at[pl.ds(first, hops * columns)]
                    group[columns * k : columns * k + columns, :] = blocks[hop][z]


def assemble(me, after, blocks):
    groups, columns, depth = blocks[0].shape
    return pl.pallas_call(
        assemble_kernel,
        out_shape=jax.ShapeDtypeStruct((len(blocks) * groups * columns, depth), jnp.bfloat16),
        in_specs=[SMEM, pl.BlockSpec(memory_space=pl.ANY)] + [VMEM] * len(blocks),
        out_specs=VMEM,
        compiler_params=pltpu.CompilerParams(vmem_limit_bytes=16 * 2**20),
        cost_estimate=pl.CostEstimate(flops=1_000_000, bytes_accessed=4_300_000, transcendentals=0),
        name="assemble",
    )(me, after, *blocks)


def project_kernel(core, attended, mine, other, out, finished, left):
    heads, depth, rows = attended.shape
    c, half = core[0], heads // 2
    steps = left.shape[0]
    step = out.shape[0] // steps

    def block(n):
        return slice(step * n, step * n + step)

    def columns(first):
        return attended[pl.ds(first, half)].reshape(half * depth, rows)

    def departure(n):
        return pltpu.make_async_copy(finished.at[block(n)], out.at[block(n)], left.at[n])

    own, rest = columns(c * half), columns((1 - c) * half)
    for n in range(steps):
        total = jnp.dot(mine[block(n), :], own, preferred_element_type=jnp.float32)
        total += jnp.dot(other[block(n), :], rest, preferred_element_type=jnp.float32)
        finished[block(n), :] = total.astype(jnp.bfloat16)
        departure(n).start()
    for n in range(steps):
        departure(n).wait()


def project(core, attended, mine, other):
    columns, _ = mine.shape
    rows, steps = attended.shape[2], 4
    return pl.pallas_call(
        project_kernel,
        out_shape=jax.ShapeDtypeStruct((columns, rows), jnp.bfloat16),
        in_specs=[SMEM, VMEM, VMEM, VMEM],
        out_specs=HBM,
        scratch_shapes=[
            pltpu.VMEM((columns, rows), jnp.bfloat16),
            pltpu.SemaphoreType.DMA((steps,)),
        ],
        compiler_params=pltpu.CompilerParams(vmem_limit_bytes=16 * 2**20),
        cost_estimate=pl.CostEstimate(
            flops=1_100_000_000, bytes_accessed=6_000_000, transcendentals=0
        ),
        name="project",
    )(core, attended, mine, other)


def body(queries, keys, values, cum_gate, out_weight):
    core, x = lax.axis_index("sp_1"), lax.axis_index("x")
    packed = pack(queries[0], keys[0], values[0])
    parts = lax.all_to_all(packed, SP, 0, 0, tiled=True)
    gate = gate_columns(cum_gate[0, 0].reshape(-1, 128))

    depth = out_weight.shape[0] // 2
    own = lax.dynamic_slice_in_dim(out_weight.T, core * depth, depth, axis=1)
    along_z = lax.all_gather(own[None], "z", axis=0, tiled=True)
    n = lax.axis_size("x")
    blocks = [along_z] + [
        lax.ppermute(along_z, "x", [(i, (i + hop) % n) for i in range(n)])
        for hop in range(1, n)
    ]
    local = attend(parts, gate)
    mine = assemble(x.reshape(1), local, blocks)
    other = lax.ppermute(mine, "sp_1", [(0, 1), (1, 0)])
    back = lax.all_to_all(local, SP, 0, 0, tiled=True)
    return project(core.reshape(1), back, mine, other).T[None]


def solution(mesh):
    split = Mesh(mesh.devices.reshape(8, 2, 12, 4), ("sp_0", "sp_1", "z", "x"))
    dp = ("z", "x")
    return jax.shard_map(
        body,
        mesh=split,
        in_specs=(P(dp, SP, None), P(dp, SP, None), P(dp, SP, None), P(dp, SP, None), P(None, dp)),
        out_specs=P(dp, SP, None),
        check_vma=False,
    )
```
